128 devices in a mesh: sp: 32 (over z, y, core), tp: 4 (over x).
Axes of the slice: x: 4, y: 4, z: 4, core: 2. Of those that a mesh axis runs over, the one named last changes fastest.
Arguments:
- tokens: bfloat16 [4, 2048, 1024], P(None, 'sp', 'tp'), may hold values from -6 to 6
- norm_gain: float32 [4, 1024], replicated, may hold values from 0.1 to 1.9
- val_weight: bfloat16 [4, 1024, 512], P(None, 'sp', 'tp'), may hold values from -0.1875 to 0.1875
- gate_weight: bfloat16 [4, 1024, 512], P(None, 'sp', 'tp'), may hold values from -0.1875 to 0.1875
- conv_taps: float32 [4, 31, 512], P(None, None, 'tp'), may hold values from -1 to 1
- conv_bias: float32 [4, 512], P(None, 'tp'), may hold values from -3 to 3
- ln_gain: float32 [4, 512], P(None, 'tp'), may hold values from 0.1 to 1.9
- ln_shift: float32 [4, 512], P(None, 'tp'), may hold values from -3 to 3
- out_weight: bfloat16 [4, 512, 1024], P(None, 'tp', 'sp'), may hold values from -0.25 to 0.25
Outputs:
- stream: bfloat16 [4, 2048, 1024], P(None, 'sp', 'tp')
The draws below stay inside these ranges and needn't reach their ends.
All inputs are finite; a program needn't handle non-finite values.
Results may differ from the reference program's by a relative error of at most 0.02.
Values may be sent and summed in bfloat16 or wider, within the bound.
A program may use at most 64 MiB of HBM per device.

```python
import jax
import jax.numpy as jnp
from jax import lax

D = 1024
CHANNELS = 512
TAPS = 31
LAYERS = 4
SEQS = 4
TOKENS = 2048


def level_of(stream_key, dims, shards, low, top_value):
    level = 1.0
    for axis_at, shards_of in shards:
        heights = jax.random.uniform(jax.random.fold_in(jax.random.fold_in(stream_key, 6), axis_at), (shards_of,), jnp.float32, low / len(shards), top_value / len(shards))
        level = level * jnp.repeat(jnp.exp(heights), dims[axis_at] // shards_of).reshape((-1,) + (1,) * (len(dims) - 1 - axis_at))
    return level


def normal_values(own_key, shape, scale, most, shards=(), dtype=jnp.bfloat16):
    result = scale * jax.random.normal(own_key, shape, jnp.float32)
    if shards:
        result = result * level_of(own_key, shape, shards, -0.22, 0.18)
    return jnp.clip(result, -most, most).astype(dtype)


def setup_inputs(seed: int = 0) -> dict:
    splits = jax.random.split(jax.random.key(seed), 10)
    tokens = normal_values(splits[0], (SEQS, TOKENS, D), 1.0, 6.0, ((1, 32), (2, 4)))
    norm_gain = jnp.clip(1.0 + 0.18 * jax.random.normal(splits[1], (LAYERS, D), jnp.float32), 0.1, 1.9)
    val_weight = normal_values(splits[2], (LAYERS, D, CHANNELS), D ** -0.5, 0.1875, ((1, 32), (2, 4)))
    gate_weight = normal_values(splits[3], (LAYERS, D, CHANNELS), D ** -0.5, 0.1875, ((1, 32), (2, 4)))
    conv_taps = normal_values(splits[4], (LAYERS, TAPS, CHANNELS), TAPS ** -0.5, 1.0, ((2, 4),), jnp.float32)
    conv_bias = normal_values(splits[5], (LAYERS, CHANNELS), 0.5, 3.0, ((1, 4),), jnp.float32)
    ln_gain = jnp.clip(1.0 + 0.18 * jax.random.normal(splits[6], (LAYERS, CHANNELS), jnp.float32), 0.1, 1.9)
    ln_shift = normal_values(splits[7], (LAYERS, CHANNELS), 0.5, 3.0, ((1, 4),), jnp.float32)
    out_weight = normal_values(splits[8], (LAYERS, CHANNELS, D), CHANNELS ** -0.5, 0.25, ((1, 4), (2, 32)))
    return {"tokens": tokens, "norm_gain": norm_gain, "val_weight": val_weight, "gate_weight": gate_weight, "conv_taps": conv_taps, "conv_bias": conv_bias, "ln_gain": ln_gain, "ln_shift": ln_shift, "out_weight": out_weight}


epsilon = 1e-06

def depthwise(padded, tap_weights, length):
    running = padded[:, 0:length] * tap_weights[0]
    for tap_idx in range(1, tap_weights.shape[0]):
        running = running + padded[:, tap_idx:tap_idx + length] * tap_weights[tap_idx]
    return running

def reference(tokens, norm_gain, val_weight, gate_weight, conv_taps, conv_bias, ln_gain, ln_shift, out_weight):
    stream = tokens
    half_width = TAPS // 2
    for layer_idx in range(LAYERS):
        widened = stream.astype(jnp.float32)
        scaled = widened * jax.lax.rsqrt(lax.optimization_barrier(jnp.mean(widened * widened, axis=-1, keepdims=True)) + epsilon)
        normed = (scaled * norm_gain[layer_idx]).astype(jnp.bfloat16)
        tok_rows = normed.reshape(-1, D)
        values = jnp.dot(tok_rows, val_weight[layer_idx], preferred_element_type=jnp.float32)
        gates = jnp.dot(tok_rows, gate_weight[layer_idx], preferred_element_type=jnp.float32)
        gated = (values * jax.nn.sigmoid(gates)).astype(jnp.bfloat16).reshape(SEQS, TOKENS, CHANNELS)
        padded = jnp.pad(gated.astype(jnp.float32), ((0, 0), (half_width, half_width), (0, 0)))
        convolved = depthwise(padded, conv_taps[layer_idx], TOKENS) + conv_bias[layer_idx]
        mean_val = lax.optimization_barrier(jnp.mean(convolved, axis=-1, keepdims=True))
        centered = convolved - mean_val
        spread = lax.optimization_barrier(jnp.mean(centered * centered, axis=-1, keepdims=True))
        normalized = centered * jax.lax.rsqrt(spread + epsilon) * ln_gain[layer_idx] + ln_shift[layer_idx]
        activated = jax.nn.silu(normalized).astype(jnp.bfloat16).reshape(-1, CHANNELS)
        branch = jnp.dot(activated, out_weight[layer_idx], preferred_element_type=jnp.float32)
        stream = (stream.astype(jnp.float32) + branch.reshape(SEQS, TOKENS, D)).astype(jnp.bfloat16)
    return stream
```

```python
from functools import partial

import jax
import jax.numpy as jnp
from jax import lax
from jax.experimental import pallas as pl
from jax.experimental.pallas import tpu as pltpu
from jax.sharding import PartitionSpec as P

MESH = pl.DeviceIdType.MESH
epsilon = 1e-06

N = 4
ORDERS = (("x", "y", "z"), ("y", "z", "x"), ("z", "x", "y"))
ALL = slice(None)


def stack_kernel(
    dims, tok_h, gain_h, val_h, gate_h, taps_h, bias_h, lng_h, lns_h, outw_h, out,
    xs, wv, wg, wo, tokb, gain, ptaps, pbias, plng, plns, ow, gs, cv, act, fin,
    loc, tsend, trecv, hsend, hrecv, psend, precv, qsend, qrecv,
    as_, ar, bs, br, cs, cr, fs, fr, ss, sr, osend, orecv,
):
    LAYERS, L, D, C, F, K, TAPS, PAD, E = dims
    SP, TP = lax.axis_size("sp"), lax.axis_size("tp")
    sp, tp = lax.axis_index("sp"), lax.axis_index("tp")
    half = TAPS // 2
    me = {"x": tp, "y": lax.rem(sp // 2, N), "z": sp // (2 * N)}
    core = lax.rem(sp, 2)
    W = (wv, wg, wo)

    def device(at, c=None):
        return (at["z"] * (2 * N) + at["y"] * 2 + (core if c is None else c), at["x"])

    def along(dim, d):
        return lax.rem(me[dim] + d + N, N)

    def neighbour(dim, d):
        return device({**me, dim: along(dim, d)})

    sibling = device(me, 1 - core)
    before = (lax.rem(sp + SP - 1, SP), tp)
    after = (lax.rem(sp + 1, SP), tp)

    def remote(src, dst, ss_, rs_, to):
        return pltpu.make_async_remote_copy(
            src_ref=src, dst_ref=dst, send_sem=ss_, recv_sem=rs_,
            device_id=to, device_id_type=MESH,
        )

    def block(k, l, at, rows=ALL):
        return W[k].at[l, at["x"], at["z"], at["y"], core, rows, :]

    started = []

    def go(c):
        c.start()
        started.append(c)
        return c

    def load(src, dst, i):
        c = pltpu.make_async_copy(src, dst, loc.at[i])
        c.start()
        return c

    own_out = load(outw_h, ow, 0)
    every = pl.ds(0, LAYERS)
    own_val = load(val_h, block(0, every, me), 1)
    own_gate = load(gate_h, block(1, every, me), 2)
    own_tok = load(tok_h, tokb, 3)

    def feat(t):
        return pl.ds(pl.multiple_of(t * F, F), F)

    own_x = load(tok_h.at[tp], xs.at[pl.ds(E, L), feat(tp)], 4)
    small_src = (bias_h, lng_h, lns_h)
    small_dst = (pbias, plng, plns)
    own_small = [load(taps_h, ptaps.at[tp], 5)]
    own_small += [load(s, d.at[tp], 6 + i) for i, (s, d) in enumerate(zip(small_src, small_dst))]
    own_gain = load(gain_h, gain, 9)

    barrier = pltpu.get_barrier_semaphore()
    peers = [neighbour(dim, d) for dim in "xyz" for d in (1, 2, 3)] + [before, after, sibling]
    for p in peers:
        pl.semaphore_signal(barrier, inc=1, device_id=p, device_id_type=MESH)

    own_out.wait()
    for l in range(LAYERS):
        piece = jnp.transpose(ow[l].astype(jnp.float32)).astype(jnp.bfloat16)
        wo[pl.ds(l, 1), pl.ds(me["x"], 1), pl.ds(me["z"], 1), pl.ds(me["y"], 1), pl.ds(core, 1)] = (
            piece.reshape(1, 1, 1, 1, 1, K, 128)
        )
    own_val.wait()
    own_gate.wait()
    own_tok.wait()
    pl.semaphore_wait(barrier, len(peers))

    JUMPS = (1, -1, 2)

    def first(k, g):
        ref = block(k, 0 if g == 0 else pl.ds(1, LAYERS - 1), me)
        return [
            remote(ref, ref, as_.at[k, g, j], ar.at[k, g, j], neighbour(ORDERS[k][0], d))
            for j, d in enumerate(JUMPS)
        ]

    def second(k, l):
        ref = block(k, l, {**me, ORDERS[k][0]: ALL})
        return [
            remote(ref, ref, bs.at[k, l, j], br.at[k, l, j], neighbour(ORDERS[k][1], d))
            for j, d in enumerate(JUMPS)
        ]

    def plane(k, i, d, rows=ALL):
        a, b, e = ORDERS[k]
        at = {a: ALL, b: pl.ds(2 * (i % 2), 2), e: along(e, d) if d else me[e]}
        return block(k, i // 2, at, rows)

    def third(k, i):
        ref = plane(k, i, 0)
        return [
            remote(ref, ref, cs.at[k, i, j], cr.at[k, i, j], neighbour(ORDERS[k][2], d))
            for j, d in enumerate((1, -1))
        ]

    def fourth(k, i):
        res = []
        for j, d in enumerate((1, -1)):
            ref = plane(k, i, -d, pl.ds(j * (K // 2), K // 2))
            res.append(
                remote(ref, ref, fs.at[k, i, j], fr.at[k, i, j], neighbour(ORDERS[k][2], d))
            )
        return res

    def across(k, i, q):
        ref = plane(k, i, (0, -1, 1, 2)[q])
        return remote(ref, ref, ss.at[k, i, q], sr.at[k, i, q], sibling)

    def send(copies):
        for c in copies:
            go(c)

    def land(copies):
        for c in copies:
            c.wait_recv()

    def open_chunk(k, i):
        send(third(k, i))
        go(across(k, i, 0))

    def advance(k, i):
        if i < 2 * LAYERS:
            land(third(k, i))
            send(fourth(k, i))
            go(across(k, i, 1))
            go(across(k, i, 2))
        if i > 0:
            land(fourth(k, i - 1))
            go(across(k, i - 1, 3))
        if i % 2 == 0:
            l = i // 2 + 1
            if l < LAYERS:
                land(second(k, l))
                open_chunk(k, 2 * l)
                open_chunk(k, 2 * l + 1)
        elif (i + 1) // 2 + 1 < LAYERS:
            send(second(k, (i + 1) // 2 + 1))

    def tick(i):
        for k in range(3):
            advance(k, i)

    def complete(k, l):
        for i in (2 * l, 2 * l + 1):
            land([across(k, i, q) for q in range(4)])

    for k in range(3):
        send(first(k, 0))

    def tok_copy(d):
        to = lax.rem(tp + d, TP)
        return remote(
            tokb.at[to], xs.at[pl.ds(E, L), feat(tp)], tsend.at[d], trecv.at[d], (sp, to)
        )

    tok_copies = [tok_copy(d) for d in range(1, TP)]
    send(tok_copies)
    for k in range(3):
        send(first(k, 1))
    for k in range(3):
        land(first(k, 0))
        send(second(k, 0))
    own_x.wait()
    land(tok_copies)
    to_before = remote(
        xs.at[pl.ds(E, L)], xs.at[pl.ds(E + L, L)], hsend.at[0], hrecv.at[0], before
    )
    to_after = remote(xs.at[pl.ds(E, L)], xs.at[pl.ds(0, L)], hsend.at[1], hrecv.at[1], after)

    @pl.when(sp > 0)
    def _():
        to_before.start()

    @pl.when(sp < SP - 1)
    def _():
        to_after.start()

    @pl.when(sp == 0)
    def _():
        xs[pl.ds(0, E), :] = jnp.zeros((E, D), xs.dtype)

    @pl.when(sp == SP - 1)
    def _():
        xs[pl.ds(E + L, E), :] = jnp.zeros((E, D), xs.dtype)

    for k in range(3):
        land(first(k, 1))
    for k in range(3):
        land(second(k, 0))
        open_chunk(k, 0)
        open_chunk(k, 1)
        send(second(k, 1))

    for c in own_small:
        c.wait()
    pair = pl.ds(core * (LAYERS // 2), LAYERS // 2)

    def taps_copy(d):
        ref = ptaps.at[tp, pair]
        return remote(ref, ref, psend.at[0, d], precv.at[0, d], (sp, lax.rem(tp + d, TP)))

    def taps_across(d):
        ref = ptaps.at[lax.rem(tp + d, TP), pair]
        return remote(ref, ref, qsend.at[d], qrecv.at[d], sibling)

    def small_copy(i, d):
        ref = small_dst[i].at[tp]
        return remote(ref, ref, psend.at[1 + i, d], precv.at[1 + i, d], (sp, lax.rem(tp + d, TP)))

    tap_copies = [taps_copy(d) for d in range(1, TP)]
    small_copies = [small_copy(i, d) for i in range(3) for d in range(1, TP)]
    tap_crossings = [taps_across(d) for d in range(1, TP)]
    send(tap_copies)
    send(small_copies)

    NC = C // 128

    def gated_part(l):
        rows, base = L + 2 * E - 2 * PAD * l, PAD * l
        x = xs[pl.ds(base, rows), :].astype(jnp.float32)
        scaled = x * lax.rsqrt(jnp.mean(x * x, axis=-1, keepdims=True) + epsilon)
        normed = (scaled * gain[pl.ds(l, 1), :]).astype(jnp.bfloat16)
        place = sp * L - E + base + lax.broadcasted_iota(jnp.int32, (rows, 128), 0)
        inside = (place >= 0) & (place < SP * L)
        for t in range(NC):
            w = jnp.concatenate([wv[l, t].reshape(D, 128), wg[l, t].reshape(D, 128)], axis=1)
            both = jnp.dot(normed, w, preferred_element_type=jnp.float32)
            v, g = both[:, :128], both[:, 128:]
            r = (v * jax.nn.sigmoid(g)).astype(jnp.bfloat16).astype(jnp.float32)
            gs[t, pl.ds(0, rows), :] = jnp.where(inside, r, 0.0)

    def conv_part(l):
        rows = L + 2 * E - 2 * PAD * (l + 1)

        def one(c, carry):
            acc = gs[c, pl.ds(PAD - half, rows), :] * ptaps[c, l, pl.ds(0, 1), :]
            for k in range(1, TAPS):
                acc = acc + gs[c, pl.ds(PAD - half + k, rows), :] * ptaps[c, l, pl.ds(k, 1), :]
            cv[c, pl.ds(0, rows), :] = acc + pbias[c, pl.ds(l, 1), :]
            return carry

        lax.fori_loop(0, NC, one, 0)
        parts = [cv[c, pl.ds(0, rows), :] for c in range(NC)]
        mean = jnp.sum(sum(parts[1:], parts[0]), axis=-1, keepdims=True) / C
        cent = [p - mean for p in parts]
        sq = [p * p for p in cent]
        inv = lax.rsqrt(jnp.sum(sum(sq[1:], sq[0]), axis=-1, keepdims=True) / C + epsilon)
        for c in range(NC):
            y = cent[c] * inv * plng[c, pl.ds(l, 1), :] + plns[c, pl.ds(l, 1), :]
            act[pl.ds(0, rows), pl.ds(c * 128, 128)] = (y * jax.nn.sigmoid(y)).astype(jnp.bfloat16)

    def project(l, n, a, base, rows):
        w = jnp.concatenate([wo[l, t, n].reshape(F, 128) for t in range(NC)], axis=1)
        y = lax.dot_general(a, w, (((1,), (1,)), ((), ())), preferred_element_type=jnp.float32)
        s = xs[pl.ds(base, rows), feat(n)].astype(jnp.float32)
        return (s + y).astype(jnp.bfloat16)

    def out_part(l):
        rows, base = L + 2 * E - 2 * PAD * (l + 1), PAD * (l + 1)
        a = act[pl.ds(0, rows), :]
        for n in range(D // F):
            xs[pl.ds(base, rows), pl.ds(n * F, F)] = project(l, n, a, base, rows)

    tick(0)
    land(tap_copies)
    send(tap_crossings)
    tick(1)
    tick(2)
    own_gain.wait()

    @pl.when(sp > 0)
    def _():
        to_after.wait_recv()

    @pl.when(sp < SP - 1)
    def _():
        to_before.wait_recv()

    for l in range(LAYERS):
        last = l == LAYERS - 1
        if last:
            for k in range(2):
                advance(k, 2 * LAYERS)
        for k in range(2):
            complete(k, l)
        gated_part(l)
        if l == 0:
            land(small_copies)
            land(tap_crossings)

            @pl.when(sp > 0)
            def _():
                to_before.wait_send()

            @pl.when(sp < SP - 1)
            def _():
                to_after.wait_send()

        if last:
            advance(2, 2 * LAYERS)
        else:
            tick(2 * l + 3)
        conv_part(l)
        complete(2, l)
        if not last:
            out_part(l)
            if 2 * l + 4 < 2 * LAYERS:
                tick(2 * l + 4)

    l = LAYERS - 1
    a = act[pl.ds(0, L), :]
    sends = []
    for d in (2, 1, 3, 0):
        n = lax.rem(tp + d, TP)
        y = project(l, n, a, E, L)
        if d == 0:
            out[pl.ds(tp, 1)] = y.reshape(1, L, F)
        else:
            fin[d] = y
            c = remote(fin.at[d], out.at[tp], osend.at[d], orecv.at[d], (sp, n))
            c.start()
            sends.append(c)
    for c in started:
        c.wait_send()
    for c in sends:
        c.wait()


def stacked(tokens, norm_gain, val_weight, gate_weight, conv_taps, conv_bias, ln_gain, ln_shift, out_weight):
    TP = lax.axis_size("tp")
    seqs, L, F = tokens.shape
    D = F * TP
    layers, K, width = val_weight.shape
    C = width * TP
    TAPS = conv_taps.shape[1]
    PAD = -(-(TAPS // 2) // 16) * 16
    E = PAD * layers
    rows = L + 2 * E
    bf16, f32 = jnp.bfloat16, jnp.float32
    dma = pltpu.SemaphoreType.DMA
    weight = pltpu.VMEM((layers, TP, N, N, 2, K, width), bf16)
    small = pltpu.VMEM((TP,) + conv_bias.shape, f32)
    return pl.pallas_call(
        partial(stack_kernel, (layers, L, D, C, F, K, TAPS, PAD, E)),
        out_shape=jax.ShapeDtypeStruct(tokens.shape, tokens.dtype),
        in_specs=[pl.BlockSpec(memory_space=pl.ANY)] * 9,
        out_specs=pl.BlockSpec(memory_space=pltpu.VMEM),
        scratch_shapes=[
            pltpu.VMEM((rows, D), bf16),
            weight, weight, weight,
            pltpu.VMEM(tokens.shape, bf16),
            pltpu.VMEM(norm_gain.shape, f32),
            pltpu.VMEM((TP,) + conv_taps.shape, f32),
            small, small, small,
            pltpu.VMEM(out_weight.shape, bf16),
            pltpu.VMEM((C // 128, rows, 128), f32),
            pltpu.VMEM((C // 128, rows, 128), f32),
            pltpu.VMEM((rows, C), bf16),
            pltpu.VMEM((TP, L, F), bf16),
            dma((10,)),
            dma((TP,)), dma((TP,)),
            dma((2,)), dma((2,)),
            dma((4, TP)), dma((4, TP)),
            dma((TP,)), dma((TP,)),
            dma((3, 2, 3)), dma((3, 2, 3)),
            dma((3, layers, 3)), dma((3, layers, 3)),
            dma((3, 2 * layers, 2)), dma((3, 2 * layers, 2)),
            dma((3, 2 * layers, 2)), dma((3, 2 * layers, 2)),
            dma((3, 2 * layers, 4)), dma((3, 2 * layers, 4)),
            dma((TP,)), dma((TP,)),
        ],
        compiler_params=pltpu.CompilerParams(
            collective_id=0, has_side_effects=True, vmem_limit_bytes=56 * 1024 * 1024
        ),
        name="stack",
    )(tokens, norm_gain, val_weight, gate_weight, conv_taps, conv_bias, ln_gain, ln_shift, out_weight)


def solution(mesh):
    placed = (
        P(None, "sp", "tp"),
        P(),
        P(None, "sp", "tp"),
        P(None, "sp", "tp"),
        P(None, None, "tp"),
        P(None, "tp"),
        P(None, "tp"),
        P(None, "tp"),
        P(None, "tp", "sp"),
    )
    return jax.shard_map(
        stacked, mesh=mesh, in_specs=placed, out_specs=P(None, "sp", "tp"), check_vma=False
    )
```

```python
from functools import partial

import jax
import jax.numpy as jnp
from jax import lax
from jax.experimental import pallas as pl
from jax.experimental.pallas import tpu as pltpu
from jax.sharding import PartitionSpec as P

MESH = pl.DeviceIdType.MESH
epsilon = 1e-06

N = 4
ORDERS = (("x", "y", "z"), ("y", "z", "x"), ("z", "x", "y"))
ALL = slice(None)


def stack_kernel(
    dims, tok_h, gain_h, val_h, gate_h, taps_h, bias_h, lng_h, lns_h, outw_h, out,
    xs, wv, wg, wo, tokb, gain, ptaps, psmall, gs, cv, act, fin,
    loc, tsend, trecv, hsend, hrecv, psend, precv, wsend, ar, br, rr, cr, fr, sr, osem,
):
    LAYERS, L, D, C, F, K, TAPS, PAD, E = dims
    SP, TP = lax.axis_size("sp"), lax.axis_size("tp")
    sp, tp = lax.axis_index("sp"), lax.axis_index("tp")
    half = TAPS // 2
    me = {"x": tp, "y": lax.rem(sp // 2, N), "z": sp // (2 * N)}
    core = lax.rem(sp, 2)
    W = (wv, wg, wo)

    def device(at, c=None):
        return (at["z"] * (2 * N) + at["y"] * 2 + (core if c is None else c), at["x"])

    def along(dim, d):
        return lax.rem(me[dim] + d + N, N)

    def neighbour(dim, d):
        return device({**me, dim: along(dim, d)})

    sibling = device(me, 1 - core)
    before = (lax.rem(sp + SP - 1, SP), tp)
    after = (lax.rem(sp + 1, SP), tp)

    def remote(src, dst, ss_, rs_, to):
        return pltpu.make_async_remote_copy(
            src_ref=src, dst_ref=dst, send_sem=ss_, recv_sem=rs_,
            device_id=to, device_id_type=MESH,
        )

    def block(k, l, at, rows=ALL):
        return W[k].at[l, at["x"], at["z"], at["y"], core, rows, :]

    started = []

    def go(c):
        c.start()
        started.append(c)
        return c

    def load(src, dst, i):
        c = pltpu.make_async_copy(src, dst, loc.at[i])
        c.start()
        return c

    every = pl.ds(0, LAYERS)
    own_out = load(outw_h, block(2, every, me), 0)
    own_val = load(val_h, block(0, every, me), 1)
    own_gate = load(gate_h, block(1, every, me), 2)
    own_tok = load(tok_h, tokb, 3)

    def feat(t):
        return pl.ds(pl.multiple_of(t * F, F), F)

    own_x = load(tok_h.at[tp], xs.at[pl.ds(E, L), feat(tp)], 4)
    small_src = (bias_h, lng_h, lns_h)
    pbias, plng, plns = small_dst = [psmall.at[i] for i in range(3)]
    own_small = [load(taps_h, ptaps.at[tp, pl.ds(0, TAPS)], 5)]
    own_small += [load(s, d.at[tp], 6 + i) for i, (s, d) in enumerate(zip(small_src, small_dst))]
    own_gain = load(gain_h, gain, 9)

    barrier = pltpu.get_barrier_semaphore()
    peers = [neighbour(dim, d) for dim in "xyz" for d in (1, 2, 3)] + [before, after, sibling]
    for p in peers:
        pl.semaphore_signal(barrier, inc=1, device_id=p, device_id_type=MESH)

    with jax.named_scope("own"):
        own_out.wait()
        own_val.wait()
        own_gate.wait()
        own_tok.wait()
    with jax.named_scope("barrier"):
        pl.semaphore_wait(barrier, len(peers))

    FIRST, SECOND, RELAY, THIRD, FOURTH, ACROSS = range(6)

    def copies_of(k, kind, rs_, moves):
        return [remote(ref, ref, wsend.at[k, kind], rs_, to) for ref, to in moves]

    def wait_blocks(k, sem, *counts):
        ref = W[k].at[tuple(pl.ds(0, n) for n in counts)]
        pltpu.make_async_copy(ref, ref, sem).wait()

    def first(k, g):
        ref = block(k, 0 if g == 0 else pl.ds(1, LAYERS - 1), me)
        return copies_of(
            k, FIRST, ar.at[k, g], [(ref, neighbour(ORDERS[k][0], d)) for d in (1, -1, 2)]
        )

    def land_first(k, g):
        wait_blocks(k, ar.at[k, g], 1 if g == 0 else LAYERS - 1, 1, 1, 3, 1)

    def second(k, l):
        ref = block(k, l, {**me, ORDERS[k][0]: ALL})
        jumps = (1, -1, 2) if l == 0 else (1, -1)
        return copies_of(
            k, SECOND, br.at[k, l], [(ref, neighbour(ORDERS[k][1], d)) for d in jumps]
        )

    def land_second(k, l):
        wait_blocks(k, br.at[k, l], 1, 1, 3 if l == 0 else 2, N, 1)

    def relay(k, l):
        a, b, _ = ORDERS[k]
        return copies_of(k, RELAY, rr.at[k, l], [
            (block(k, l, {**me, a: ALL, b: along(b, -d)}, halves[j]), neighbour(b, d))
            for j, d in enumerate((1, -1))
        ])

    def land_relay(k, l):
        wait_blocks(k, rr.at[k, l], 1, 1, 1, N, 1)

    def plane(k, i, d, rows=ALL):
        a, b, e = ORDERS[k]
        at = {a: ALL, b: pl.ds(2 * (i % 2), 2), e: along(e, d) if d else me[e]}
        return block(k, i // 2, at, rows)

    def third(k, i):
        return copies_of(k, THIRD, cr.at[k, i], [
            (plane(k, i, 0), neighbour(ORDERS[k][2], d)) for d in (1, -1)
        ])

    def land_third(k, i):
        wait_blocks(k, cr.at[k, i], 1, 1, 2, N, 2)

    def fourth(k, i):
        return copies_of(k, FOURTH, fr.at[k, i], [
            (plane(k, i, -d, halves[j]), neighbour(ORDERS[k][2], d)) for j, d in enumerate((1, -1))
        ])

    def land_fourth(k, i):
        wait_blocks(k, fr.at[k, i], 1, 1, 2, N, 1)

    def across(k, i, d):
        return copies_of(k, ACROSS, sr.at[k, i // 2], [(plane(k, i, d), sibling)])

    def complete(k, l):
        wait_blocks(k, sr.at[k, l], 1, 2, N, N, 2)

    halves = (pl.ds(0, K // 2), pl.ds(K // 2, K // 2))

    def send(copies):
        for c in copies:
            c.start()

    def open_chunk(k, i):
        send(third(k, i))
        send(across(k, i, 0))

    def pass_on(k, i):
        land_third(k, i)
        send(fourth(k, i))
        send(across(k, i, -1))
        send(across(k, i, 1))

    def finish_chunk(k, i):
        land_fourth(k, i)
        send(across(k, i, 2))

    def tick(i, opened=(), relayed=None):
        with jax.named_scope(f"tick{i}"):
            for k in range(3):
                if i < 2 * LAYERS:
                    pass_on(k, i)
                if relayed is not None:
                    land_relay(k, relayed)
                for j in opened:
                    open_chunk(k, j)
                if i >= 2:
                    finish_chunk(k, i - 2)

    for k in range(3):
        send(first(k, 0))
    for k in range(3):
        send(first(k, 1))

    tok_copies = [
        remote(
            tokb.at[lax.rem(tp + d, TP)], xs.at[pl.ds(E, L), feat(tp)],
            tsend.at[0], trecv.at[0], (sp, lax.rem(tp + d, TP)),
        )
        for d in range(1, TP)
    ]
    tok_all = tokb.at[pl.ds(0, TP - 1)]
    send(tok_copies)
    with jax.named_scope("first0"):
        for k in range(3):
            land_first(k, 0)
            send(second(k, 0))
    with jax.named_scope("first1"):
        for k in range(3):
            land_first(k, 1)
            send(second(k, 1))
        for l in range(2, LAYERS):
            for k in range(3):
                send(second(k, l))
    with jax.named_scope("tokens"):
        own_x.wait()
        pltpu.make_async_copy(tok_all, tok_all, trecv.at[0]).wait()
    to_before = remote(
        xs.at[pl.ds(E, L)], xs.at[pl.ds(E + L, L)], hsend.at[0], hrecv.at[0], before
    )
    to_after = remote(xs.at[pl.ds(E, L)], xs.at[pl.ds(0, L)], hsend.at[1], hrecv.at[1], after)

    @pl.when(sp > 0)
    def _():
        to_before.start()

    @pl.when(sp < SP - 1)
    def _():
        to_after.start()

    @pl.when(sp == 0)
    def _():
        xs[pl.ds(0, E), :] = jnp.zeros((E, D), xs.dtype)

    @pl.when(sp == SP - 1)
    def _():
        xs[pl.ds(E + L, E), :] = jnp.zeros((E, D), xs.dtype)

    with jax.named_scope("second0"):
        for k in range(3):
            land_second(k, 1)
            send(relay(k, 1))
            land_second(k, 0)
            open_chunk(k, 0)
            open_chunk(k, 1)
    with jax.named_scope("second2"):
        for l in range(2, LAYERS):
            for k in range(3):
                land_second(k, l)
                send(relay(k, l))

    for c in own_small:
        c.wait()

    part = pl.ds(core * (ptaps.shape[1] // 2), ptaps.shape[1] // 2)
    for k in range(TAPS, ptaps.shape[1]):
        ptaps[pl.ds(tp, 1), k] = jnp.zeros((1,) + ptaps.shape[2:], ptaps.dtype)

    others = [lax.rem(tp + d, TP) for d in range(1, TP)]
    tap_ref = ptaps.at[tp, part]
    tap_copies = [remote(tap_ref, tap_ref, psend.at[0], precv.at[0], (sp, t)) for t in others]
    small_copies = [
        remote(d.at[tp], d.at[tp], psend.at[1], precv.at[1], (sp, t))
        for d in small_dst for t in others
    ]
    tap_crossings = [
        remote(ptaps.at[t, part], ptaps.at[t, part], psend.at[2], precv.at[2], sibling)
        for t in others
    ]
    tap_all = ptaps.at[pl.ds(0, TP - 1), part]
    small_all = psmall.at[:, pl.ds(0, TP - 1)]

    def wait_for(ref, sem):
        pltpu.make_async_copy(ref, ref, sem).wait()

    send(tap_copies)
    send(small_copies)

    NC = C // 128

    def gated_part(l):
        rows, base = L + 2 * E - 2 * PAD * l, PAD * l
        x = xs[pl.ds(base, rows), :].astype(jnp.float32)
        scaled = x * lax.rsqrt(jnp.mean(x * x, axis=-1, keepdims=True) + epsilon)
        normed = (scaled * gain[pl.ds(l, 1), :]).astype(jnp.bfloat16)
        place = sp * L - E + base + lax.broadcasted_iota(jnp.int32, (rows, 128), 0)
        inside = (place >= 0) & (place < SP * L)
        for t in range(NC):
            w = jnp.concatenate([wv[l, t].reshape(D, 128), wg[l, t].reshape(D, 128)], axis=1)
            both = jnp.dot(normed, w, preferred_element_type=jnp.float32)
            v, g = both[:, :128], both[:, 128:]
            r = (v * jax.nn.sigmoid(g)).astype(jnp.bfloat16).astype(jnp.float32)
            gs[t, pl.ds(0, rows), :] = jnp.where(inside, r, 0.0)

    def conv_part(l):
        rows = L + 2 * E - 2 * PAD * (l + 1)

        def one(c, carry):
            acc = gs[c, pl.ds(PAD - half, rows), :] * ptaps[c, 0, pl.ds(l, 1), :]
            for k in range(1, TAPS):
                acc = acc + gs[c, pl.ds(PAD - half + k, rows), :] * ptaps[c, k, pl.ds(l, 1), :]
            cv[c, pl.ds(0, rows), :] = acc + pbias[c, pl.ds(l, 1), :]
            return carry

        lax.fori_loop(0, NC, one, 0)
        parts = [cv[c, pl.ds(0, rows), :] for c in range(NC)]
        mean = jnp.sum(sum(parts[1:], parts[0]), axis=-1, keepdims=True) / C
        cent = [p - mean for p in parts]
        sq = [p * p for p in cent]
        inv = lax.rsqrt(jnp.sum(sum(sq[1:], sq[0]), axis=-1, keepdims=True) / C + epsilon)
        for c in range(NC):
            y = cent[c] * inv * plng[c, pl.ds(l, 1), :] + plns[c, pl.ds(l, 1), :]
            act[pl.ds(0, rows), pl.ds(c * 128, 128)] = (y * jax.nn.sigmoid(y)).astype(jnp.bfloat16)

    def project(l, n, a, base, rows):
        w = jnp.concatenate([wo[l, t, n].reshape(F, 128) for t in range(NC)], axis=1)
        y = lax.dot_general(a, w, (((1,), (1,)), ((), ())), preferred_element_type=jnp.float32)
        s = xs[pl.ds(base, rows), feat(n)].astype(jnp.float32)
        return (s + y).astype(jnp.bfloat16)

    def out_part(l):
        rows, base = L + 2 * E - 2 * PAD * (l + 1), PAD * (l + 1)
        a = act[pl.ds(0, rows), :]
        for n in range(D // F):
            xs[pl.ds(base, rows), pl.ds(n * F, F)] = project(l, n, a, base, rows)

    tick(0, (2, 3), 1)
    wait_for(tap_all, precv.at[0])
    send(tap_crossings)
    tick(1, (4,), 2)
    tick(2, (5,))
    tick(3, (6,), 3)
    tick(4, (7,))
    own_gain.wait()

    @pl.when(sp > 0)
    def _():
        to_after.wait_recv()

    @pl.when(sp < SP - 1)
    def _():
        to_before.wait_recv()

    for l in range(LAYERS):
        last = l == LAYERS - 1
        with jax.named_scope("arrive"):
            for k in range(2):
                complete(k, l)
        with jax.named_scope("gated"):
            gated_part(l)
        if l == 0:
            wait_for(small_all, precv.at[1])
            wait_for(tap_all, precv.at[2])

            @pl.when(sp > 0)
            def _():
                to_before.wait_send()

            @pl.when(sp < SP - 1)
            def _():
                to_after.wait_send()

        if 2 * l + 5 < 2 * LAYERS + 2:
            tick(2 * l + 5)
        with jax.named_scope("conv"):
            conv_part(l)
        with jax.named_scope("arrive2"):
            complete(2, l)
        if not last:
            with jax.named_scope("project"):
                out_part(l)
            if 2 * l + 6 < 2 * LAYERS + 2:
                tick(2 * l + 6)

    l = LAYERS - 1
    a = act[pl.ds(0, L), :]
    with jax.named_scope("finish"):
        for d in (2, 1, 3, 0):
            n = lax.rem(tp + d, TP)
            y = project(l, n, a, E, L)
            if d == 0:
                out[pl.ds(tp, 1)] = y.reshape(1, L, F)
            else:
                fin[d] = y
                send([remote(fin.at[d], out.at[tp], osem.at[0], osem.at[1], (sp, n))])
    with jax.named_scope("drain"):
        for k in range(3):
            wait_blocks(k, wsend.at[k, FIRST], LAYERS, 1, 1, 3, 1)
            wait_blocks(k, wsend.at[k, SECOND], LAYERS - 1, 1, 3, N, 1)
            wait_blocks(k, wsend.at[k, RELAY], LAYERS - 1, 1, 1, N, 1)
            wait_blocks(k, wsend.at[k, THIRD], 1, N, N, N, 2)
            wait_blocks(k, wsend.at[k, FOURTH], 1, 2, N, N, 2)
            wait_blocks(k, wsend.at[k, ACROSS], 2, N, N, N, 2)
        wait_for(tok_all, tsend.at[0])
        wait_for(tap_all, psend.at[0])
        wait_for(small_all, psend.at[1])
        wait_for(tap_all, psend.at[2])
        fin_all = fin.at[pl.ds(1, TP - 1)]
        wait_for(fin_all, osem.at[0])
        wait_for(fin_all, osem.at[1])


def stacked(tokens, norm_gain, val_weight, gate_weight, conv_taps, conv_bias, ln_gain, ln_shift, out_weight):
    TP = lax.axis_size("tp")
    seqs, L, F = tokens.shape
    D = F * TP
    layers, K, width = val_weight.shape
    C = width * TP
    TAPS = conv_taps.shape[1]
    PAD = -(-(TAPS // 2) // 16) * 16
    E = PAD * layers
    rows = L + 2 * E
    bf16, f32 = jnp.bfloat16, jnp.float32
    dma = pltpu.SemaphoreType.DMA
    weight = pltpu.VMEM((layers, TP, N, N, 2, K, width), bf16)
    return pl.pallas_call(
        partial(stack_kernel, (layers, L, D, C, F, K, TAPS, PAD, E)),
        out_shape=jax.ShapeDtypeStruct(tokens.shape, tokens.dtype),
        in_specs=[pl.BlockSpec(memory_space=pl.ANY)] * 9,
        out_specs=pl.BlockSpec(memory_space=pltpu.VMEM),
        scratch_shapes=[
            pltpu.VMEM((rows, D), bf16),
            weight, weight, weight,
            pltpu.VMEM(tokens.shape, bf16),
            pltpu.VMEM(norm_gain.shape, f32),
            pltpu.VMEM((TP, 2 * ((TAPS + 1) // 2), layers, width), f32),
            pltpu.VMEM((3, TP) + conv_bias.shape, f32),
            pltpu.VMEM((C // 128, rows, 128), f32),
            pltpu.VMEM((C // 128, rows, 128), f32),
            pltpu.VMEM((rows, C), bf16),
            pltpu.VMEM((TP, L, F), bf16),
            dma((10,)),
            dma((1,)), dma((1,)),
            dma((2,)), dma((2,)),
            dma((3,)), dma((3,)),
            dma((3, 6)),
            dma((3, 2)),
            dma((3, layers)),
            dma((3, layers)),
            dma((3, 2 * layers)),
            dma((3, 2 * layers)),
            dma((3, layers)),
            dma((2,)),
        ],
        compiler_params=pltpu.CompilerParams(
            collective_id=0, has_side_effects=True, vmem_limit_bytes=56 * 1024 * 1024
        ),
        name="stack",
    )(
        tokens, norm_gain, val_weight, gate_weight, jnp.swapaxes(conv_taps, 0, 1), conv_bias,
        ln_gain, ln_shift, jnp.swapaxes(out_weight, 1, 2),
    )


def solution(mesh):
    placed = (
        P(None, "sp", "tp"),
        P(),
        P(None, "sp", "tp"),
        P(None, "sp", "tp"),
        P(None, None, "tp"),
        P(None, "tp"),
        P(None, "tp"),
        P(None, "tp"),
        P(None, "tp", "sp"),
    )
    return jax.shard_map(
        stacked, mesh=mesh, in_specs=placed, out_specs=P(None, "sp", "tp"), check_vma=False
    )
```
